128 devices in a mesh: ra: 16 (over z, x), cb: 8 (over y, core).
Axes of the slice: x: 4, y: 4, z: 4, core: 2. Of those that a mesh axis runs over, the one named last changes fastest.
Arguments:
- tokens: bfloat16 [512, 3072], P(None, 'ra'), may hold values from -14 to 14, as said below
- norm_gain: float32 [2, 3072], P(None, 'ra'), may hold values from 0.1 to 1.9
- gate_weight: float32 [2, 3072, 8448], P(None, 'ra', 'cb'), may hold values from -0.109375 to 0.109375
- gate_scale: float32 [2, 8448], P(None, 'cb'), may hold values from 0.5 to 2
- value_weight: float32 [2, 3072, 8448], P(None, 'ra', 'cb'), may hold values from -0.109375 to 0.109375
- value_scale: float32 [2, 8448], P(None, 'cb'), may hold values from 0.5 to 2
- gate_conv: float32 [2, 3, 8448], P(None, None, 'cb'), may hold values from -3.5 to 3.5
- value_conv: float32 [2, 3, 8448], P(None, None, 'cb'), may hold values from -3.5 to 3.5
- gate_bias: float32 [2, 8448], P(None, 'cb'), may hold values from -3 to 3
- value_bias: float32 [2, 8448], P(None, 'cb'), may hold values from -3 to 3
- down_weight: float32 [2, 8448, 3072], P(None, 'cb', 'ra'), may hold values from -0.0625 to 0.0625
- down_scale: float32 [2, 3072], P(None, 'ra'), may hold values from 0.5 to 2
Outputs:
- stream_out: bfloat16 [512, 3072], P(None, 'ra')
The draws below stay inside these ranges and needn't reach their ends.
Inputs may be any that keep to these rules, and one draw needn't show every extreme that they name: `tokens`: real values; within each token, the blocks of D // 16 consecutive features have scales that differ.
All inputs are finite; a program needn't handle non-finite values.
Results may differ from the reference program's by a relative error of at most 0.039.
Values may be sent and summed in bfloat16 or wider, within the bound.
A program may use at most 64 MiB of HBM per device.

```python
import math
import jax
import jax.numpy as jnp
from jax import lax

D = 3072
FF = 8448
TAPS = 3
LAYERS = 2
SEQ_LEN = 8
TOKENS = 512
N_CB = 8


def draw_tokens(key, part):
    first, second, third = jax.random.split(key, 3)
    scales = jnp.exp(jax.random.uniform(second, (TOKENS, 16), jnp.float32, -1.2, 1.2))
    widths = jnp.repeat(scales, D // 16, axis=1)
    base = jnp.clip(jax.random.normal(first, (TOKENS, D), jnp.float32), -4.0, 4.0)
    return (base * widths).astype(jnp.bfloat16)


def levels(own_key, dims, shards, smallest, top_value):
    loudness = 1.0
    for position, parts in shards:
        draws = jax.random.uniform(jax.random.fold_in(jax.random.fold_in(own_key, 6), position), (parts,), jnp.float32, smallest / len(shards), top_value / len(shards))
        loudness = loudness * jnp.repeat(jnp.exp(draws), dims[position] // parts).reshape((-1,) + (1,) * (len(dims) - 1 - position))
    return loudness


def centred(own_key, shape, scale, bound, cuts=(), kind=jnp.bfloat16):
    result = scale * jax.random.normal(own_key, shape, jnp.float32)
    if cuts:
        result = result * levels(own_key, shape, cuts, -0.22, 0.18)
    return jnp.clip(result, -bound, bound).astype(kind)


def setup_inputs(seed: int = 0) -> dict:
    arg_keys = jax.random.split(jax.random.key(seed), 13)
    tokens = draw_tokens(jax.random.fold_in(arg_keys[12], 71), 0)
    norm_gain = jnp.clip(1.0 + 0.18 * jax.random.normal(arg_keys[1], (LAYERS, D), jnp.float32), 0.1, 1.9)
    gate_weight = centred(arg_keys[2], (LAYERS, D, FF), D ** -0.5, 0.109375, ((1, 16), (2, 8)), jnp.float32)
    gate_scale = jnp.clip(jnp.exp(math.log(2.0) - 1.3862944 * jax.random.uniform(arg_keys[3], (LAYERS, FF), jnp.float32) ** levels(arg_keys[3], (LAYERS, FF), ((1, 8),), -0.2, 0.2)), 0.5, 2.0)
    value_weight = centred(arg_keys[4], (LAYERS, D, FF), D ** -0.5, 0.109375, ((1, 16), (2, 8)), jnp.float32)
    value_scale = jnp.clip(jnp.exp(math.log(2.0) - 1.3862944 * jax.random.uniform(arg_keys[5], (LAYERS, FF), jnp.float32) ** levels(arg_keys[5], (LAYERS, FF), ((1, 8),), -0.2, 0.2)), 0.5, 2.0)
    gate_conv = centred(arg_keys[6], (LAYERS, TAPS, FF), TAPS ** -0.5, 3.5, ((2, 8),), jnp.float32)
    value_conv = centred(arg_keys[7], (LAYERS, TAPS, FF), TAPS ** -0.5, 3.5, ((2, 8),), jnp.float32)
    gate_bias = centred(arg_keys[8], (LAYERS, FF), 0.5, 3.0, ((1, 8),), jnp.float32)
    value_bias = centred(arg_keys[9], (LAYERS, FF), 0.5, 3.0, ((1, 8),), jnp.float32)
    down_weight = centred(arg_keys[10], (LAYERS, FF, D), FF ** -0.5, 0.0625, ((1, 8), (2, 16)), jnp.float32)
    down_scale = jnp.clip(jnp.exp(math.log(2.0) - 1.3862944 * jax.random.uniform(arg_keys[11], (LAYERS, D), jnp.float32) ** levels(arg_keys[11], (LAYERS, D), ((1, 16),), -0.2, 0.2)), 0.5, 2.0)
    return {"tokens": tokens, "norm_gain": norm_gain, "gate_weight": gate_weight, "gate_scale": gate_scale, "value_weight": value_weight, "value_scale": value_scale, "gate_conv": gate_conv, "value_conv": value_conv, "gate_bias": gate_bias, "value_bias": value_bias, "down_weight": down_weight, "down_scale": down_scale}


epsilon = 1e-06
residual_keep = 0.5

def causal_conv(values, conv_taps, conv_bias):
    row_count, col_count = values.shape
    blocks = values.reshape(row_count // SEQ_LEN, SEQ_LEN, col_count)
    padded = jnp.pad(blocks, ((0, 0), (TAPS - 1, 0), (0, 0)))
    summed = conv_bias + jnp.zeros_like(blocks)
    for offset in range(TAPS):
        summed = summed + padded[:, offset:offset + SEQ_LEN] * conv_taps[offset]
    return summed.reshape(row_count, col_count)

def reference(tokens, norm_gain, gate_weight, gate_scale, value_weight, value_scale, gate_conv, value_conv, gate_bias, value_bias, down_weight, down_scale):
    stream = tokens
    for depth_index in range(LAYERS):
        widened = stream.astype(jnp.float32)
        squares = lax.optimization_barrier(jnp.sum(widened * widened, axis=1, keepdims=True))
        inverse_rms = lax.rsqrt(squares / D + epsilon)
        normed = (widened * norm_gain[depth_index]).astype(jnp.bfloat16)
        gate_pre = jnp.dot(normed, gate_weight[depth_index].astype(jnp.bfloat16), preferred_element_type=jnp.float32) * inverse_rms * gate_scale[depth_index]
        value_pre = jnp.dot(normed, value_weight[depth_index].astype(jnp.bfloat16), preferred_element_type=jnp.float32) * inverse_rms * value_scale[depth_index]
        gate_mixed = causal_conv(gate_pre, gate_conv[depth_index], gate_bias[depth_index])
        value_mixed = causal_conv(value_pre, value_conv[depth_index], value_bias[depth_index])
        hidden = (jax.nn.silu(gate_mixed) * value_mixed).astype(jnp.bfloat16)
        hidden = lax.optimization_barrier(hidden)
        pieces = hidden.astype(jnp.float32).reshape(TOKENS, N_CB, FF // N_CB)
        down_half = lax.optimization_barrier(down_weight[depth_index].astype(jnp.bfloat16))
        down_pieces = down_half.astype(jnp.float32).reshape(N_CB, FF // N_CB, D)
        partial_value = jnp.einsum('tcf,cfd->ctd', pieces, down_pieces)
        rounded = lax.optimization_barrier(partial_value.astype(jnp.bfloat16)).astype(jnp.float32)
        branch = lax.optimization_barrier(jnp.sum(rounded, axis=0)) * down_scale[depth_index]
        stream = (residual_keep * widened + branch).astype(jnp.bfloat16)
    return stream
```

```python
import functools

import jax
import jax.numpy as jnp
from jax import lax
from jax.experimental import pallas as pl
from jax.experimental.pallas import tpu as pltpu
from jax.sharding import PartitionSpec as P

D = 3072
TAPS = 3
LAYERS = 2
SEQ_LEN = 8
epsilon = 1e-06
residual_keep = 0.5

MESH = pl.DeviceIdType.MESH
F32 = jnp.float32
BF16 = jnp.bfloat16

TOK = 256
ROWS = 16
W = 192
FFD = 1056
MAIN = 512
LEFT = FFD - 2 * MAIN
PRE = (2 * MAIN + 128, 2 * MAIN, 2 * MAIN + 128, 2 * MAIN)
HID = (MAIN + 128, MAIN, MAIN + 128, MAIN)
ORDER = ((0, 1, 2, 3), (1, 0, 3, 2), (2, 3, 0, 1), (3, 2, 1, 0))
CH = range(4)


def pick(axis, index, rank):
    return tuple(index if i == axis else slice(None) for i in range(rank))


def kernel(
    tokens,
    norm_gain,
    gate_weight,
    gate_scale,
    value_weight,
    value_scale,
    gate_conv,
    value_conv,
    gate_bias,
    value_bias,
    down_weight,
    down_scale,
    out,
    *scratch,
):
    it = iter(scratch)
    take = lambda n: [next(it) for _ in range(n)]
    (stream, squares, normed, gain, dscale) = take(5)
    (wide, dwide) = take(2)
    wcols = take(2)
    drows = take(2)
    params = take(6)
    snd = [take(4) for _ in range(4)]
    kept = [take(4) for _ in range(4)]
    got = [take(4) for _ in range(4)]
    hid = take(4)
    (total, ysend, yrecv) = take(3)
    (load_sem, peer_send, peer_recv, rs_send, rs_recv, ag_send, ag_recv, y_send, y_recv, out_sem) = take(10)

    ra = lax.axis_index("ra")
    cb = lax.axis_index("cb")
    x, z = ra % 4, ra // 4
    y, c = cb // 2, cb % 2

    def at(nx, nz):
        return nz * 4 + nx

    def flip(v):
        return v + 1 - 2 * (v % 2)

    def choose(first, second):
        return first * (1 - c) + second * c

    xa, xb, za, zb = at(flip(x), z), at(3 - x, z), at(x, flip(z)), at(x, 3 - z)
    bxa, bxb, bza, bzb = ((x + 1) // 2) % 2, x // 2, ((z + 1) // 2) % 2, z // 2
    mates = (choose(xa, zb), choose(xb, za), choose(za, xb), choose(zb, xa))
    bits = (choose(bxa, bzb), choose(bxb, bza), choose(bza, bxb), choose(bzb, bxa))
    peer = (ra, y * 2 + 1 - c)
    ymates = ((ra, flip(y) * 2 + c), (ra, (3 - y) * 2 + c))

    sources = (gate_scale, value_scale, gate_conv, value_conv, gate_bias, value_bias)
    loads = {}

    def load(name, src, dst, index):
        loads[name] = pltpu.make_async_copy(src, dst, load_sem.at[index])
        loads[name].start()

    load("x", tokens.at[pl.ds(c * 16, 16)], stream, 0)
    load("gain", norm_gain, gain, 1)
    for layer in range(LAYERS):
        load(("g", layer), gate_weight.at[layer], wide.at[layer, 0], 2 + layer * 3)
        load(("v", layer), value_weight.at[layer], wide.at[layer, 1], 3 + layer * 3)
        load(("d", layer), down_weight.at[layer], dwide.at[layer], 4 + layer * 3)
        if layer == 0:
            load("ds", down_scale, dscale, 8)
            for i, src in enumerate(sources):
                load(("p", i), src, params[i].at[0], 9 + i)

    barrier = pltpu.get_barrier_semaphore()
    for mate in mates:
        pl.semaphore_signal(barrier, inc=1, device_id=(mate, cb), device_id_type=MESH)
    for target in (peer, *ymates):
        pl.semaphore_signal(barrier, inc=1, device_id=target, device_id_type=MESH)

    sent = []

    def remote(src, dst, send_sem, recv_sem, target):
        copy = pltpu.make_async_remote_copy(
            src_ref=src, dst_ref=dst, send_sem=send_sem, recv_sem=recv_sem,
            device_id=target, device_id_type=MESH,
        )
        copy.start()
        sent.append(copy)
        return copy

    line = lax.broadcasted_iota(jnp.int32, (LEFT, 128), 1)
    row = lax.broadcasted_iota(jnp.int32, (LEFT, 128), 0)
    put_gate = (line == row).astype(F32).astype(BF16)
    put_value = (line == row + LEFT).astype(F32).astype(BF16)

    def cast_up(layer):
        loads[("g", layer)].wait()
        loads[("v", layer)].wait()
        g, v = wide.at[layer, 0], wide.at[layer, 1]
        wcols[0][layer, 0, :, 0:MAIN] = g[:, 0:MAIN].astype(BF16)
        wcols[0][layer, 0, :, MAIN : 2 * MAIN] = v[:, 0:MAIN].astype(BF16)
        low = jnp.dot(g[:, 2 * MAIN : FFD].astype(BF16), put_gate, preferred_element_type=F32)
        low += jnp.dot(v[:, 2 * MAIN : FFD].astype(BF16), put_value, preferred_element_type=F32)
        wcols[0][layer, 0, :, 2 * MAIN : 2 * MAIN + 128] = low.astype(BF16)
        wcols[1][layer, 0, :, 0:MAIN] = g[:, MAIN : 2 * MAIN].astype(BF16)
        wcols[1][layer, 0, :, MAIN : 2 * MAIN] = v[:, MAIN : 2 * MAIN].astype(BF16)

    def cast_down(layer):
        loads[("d", layer)].wait()
        d = dwide.at[layer]
        drows[0][layer, 0, 0:MAIN, :] = d[0:MAIN, :].astype(BF16)
        drows[0][layer, 0, MAIN : MAIN + LEFT, :] = d[2 * MAIN : FFD, :].astype(BF16)
        drows[0][layer, 0, MAIN + LEFT : MAIN + 128, :] = jnp.zeros((128 - LEFT, W), BF16)
        drows[1][layer, 0, :, :] = d[MAIN : 2 * MAIN, :].astype(BF16)

    from_peer = {}

    def give(name, ref_from, ref_to, index):
        from_peer[name] = remote(ref_from, ref_to, peer_send.at[index], peer_recv.at[index], peer)

    def need(name):
        if name in from_peer:
            from_peer.pop(name).wait_recv()

    lane = lax.broadcasted_iota(jnp.int32, (TOK, 128), 1)

    def prepare(layer):
        wideal = stream[...].reshape(TOK, W).astype(F32)
        own = jnp.sum(wideal * wideal, axis=1, keepdims=True)
        squares[...] = jnp.where(lane == 2 * LEFT, own, 0.0).reshape(squares.shape)
        normed[...] = (wideal * gain[layer : layer + 1, :]).astype(BF16).reshape(normed.shape)

    def project(layer, k, index):
        rows = normed[index].reshape(TOK // 2, W)
        product = jnp.dot(rows, wcols[k % 2][layer, k // 2], preferred_element_type=F32)
        if k == 0:
            tail = product[:, 2 * MAIN :] + squares[index].reshape(TOK // 2, 128)
            return product[:, : 2 * MAIN], tail
        return product, None

    def store(ref, value):
        main, tail = value
        lead = ref.shape[:-1]
        if tail is None:
            ref[...] = main.astype(BF16).reshape(ref.shape)
        else:
            ref[..., 0 : 2 * MAIN] = main.astype(BF16).reshape(*lead, 2 * MAIN)
            ref[..., 2 * MAIN :] = tail.astype(BF16).reshape(*lead, 128)

    def rs_copy(layer, step, k):
        dim = ORDER[k][step]
        return remote(
            snd[step][k].at[layer], got[step][k].at[layer],
            rs_send.at[layer, step, k], rs_recv.at[layer, step, k], (mates[dim], cb),
        )

    keep_row = lax.broadcasted_iota(jnp.int32, (ROWS, 1), 0) % SEQ_LEN

    def mix(pre, taps, bias):
        back_one = jnp.where(keep_row >= 1, pltpu.roll(pre, 1, 0), 0.0)
        back_two = jnp.where(keep_row >= 2, pltpu.roll(pre, 2, 0), 0.0)
        return bias + back_two * taps[0] + back_one * taps[1] + pre * taps[2]

    def gated(layer, slot, cols, gate_sum, value_sum, inverse):
        scale_g, scale_v, conv_g, conv_v, bias_g, bias_v = params
        one = lambda ref: ref[slot, layer : layer + 1, cols]
        taps = lambda ref: [ref[slot, layer, i : i + 1, cols] for i in range(TAPS)]
        gate = mix(gate_sum * inverse * one(scale_g), taps(conv_g), one(bias_g))
        value = mix(value_sum * inverse * one(scale_v), taps(conv_v), one(bias_v))
        return (gate / (1.0 + jnp.exp(-gate)) * value).astype(BF16)

    loads["x"].wait()
    loads["gain"].wait()
    for layer in range(LAYERS):
        prepare(layer)
        if layer == 0:
            cast_up(0)
            pl.semaphore_wait(barrier, 7)
            for i in range(2):
                give(("w", i, 0), wcols[i].at[0, 0], wcols[i].at[0, 1], i)
        flights = {}
        for k in CH:
            if k >= 2:
                need(("w", k - 2, layer))
            dim = ORDER[k][0]
            store(snd[0][k].at[layer], project(layer, k, pick(dim, 1 - bits[dim], 4)))
            flights[k] = rs_copy(layer, 0, k)
        for k in CH:
            dim = ORDER[k][0]
            store(kept[0][k].at[layer], project(layer, k, pick(dim, bits[dim], 4)))
        if layer == 0:
            cast_down(0)
            for i in range(2):
                give(("d", i, 0), drows[i].at[0, 0], drows[i].at[0, 1], 4 + i)
            loads["ds"].wait()
            for i in range(6):
                loads[("p", i)].wait()
                give(("p", i), params[i].at[0], params[i].at[1], 8 + i)
            cast_up(1)
            for i in range(2):
                give(("w", i, 1), wcols[i].at[1, 0], wcols[i].at[1, 1], 2 + i)
            cast_down(1)
            for i in range(2):
                give(("d", i, 1), drows[i].at[1, 0], drows[i].at[1, 1], 6 + i)
        for step in range(1, 4):
            for k in CH:
                left = sorted(ORDER[k][step - 1 :])
                left.remove(ORDER[k][step - 1])
                dim = ORDER[k][step]
                axis = left.index(dim)
                rank = len(left)
                flights[k].wait_recv()
                away, home = pick(axis, 1 - bits[dim], rank), pick(axis, bits[dim], rank)
                before, arrived = kept[step - 1][k].at[layer], got[step - 1][k].at[layer]
                snd[step][k][layer] = before[away] + arrived[away]
                flights[k] = rs_copy(layer, step, k)
                kept[step][k][layer] = before[home] + arrived[home]
        if layer == 0:
            for i in range(6):
                need(("p", i))
        inverse = None
        for k in CH:
            slot, part = k // 2, k % 2
            flights[k].wait_recv()
            final = kept[3][k][layer].astype(F32) + got[3][k][layer].astype(F32)
            if k == 0:
                low = final[:, 2 * MAIN :]
                own_lane = lax.broadcasted_iota(jnp.int32, (ROWS, 128), 1) == 2 * LEFT
                mean = jnp.sum(jnp.where(own_lane, low, 0.0), axis=1, keepdims=True) / D
                inverse = lax.rsqrt(mean + epsilon)
            mine = tuple(bits)
            cols = slice(part * MAIN, (part + 1) * MAIN)
            hid[k][(layer, *mine, slice(None), slice(0, MAIN))] = gated(
                layer, slot, cols, final[:, 0:MAIN], final[:, MAIN : 2 * MAIN], inverse
            )
            if part == 0:
                low = final[:, 2 * MAIN :]
                high = pltpu.roll(low, 128 - LEFT, 1)
                hid[k][(layer, *mine, slice(None), slice(MAIN, MAIN + 128))] = jnp.zeros((ROWS, 128), BF16)
                hid[k][(layer, *mine, slice(None), slice(MAIN, MAIN + LEFT))] = gated(
                    layer, slot, slice(2 * MAIN, FFD), low[:, 0:LEFT], high[:, 0:LEFT], inverse
                )
            flights[k] = gather(layer, 3, k, hid, bits, mates, cb, ag_send, ag_recv, remote)
        for step in (2, 1, 0):
            for k in CH:
                flights[k].wait_recv()
                flights[k] = gather(layer, step, k, hid, bits, mates, cb, ag_send, ag_recv, remote)
        for k in CH:
            if k >= 2:
                need(("d", k - 2, layer))
            flights[k].wait_recv()
            part = jnp.dot(
                hid[k][layer].reshape(TOK, HID[k]), drows[k % 2][layer, k // 2], preferred_element_type=F32
            )
            if k == 0:
                total[...] = part
            elif k < 3:
                total[...] += part
            else:
                ysend[layer, 0] = (total[...] + part).astype(BF16).reshape(2, TOK // 2, W)
        hops = [
            remote(
                ysend.at[layer, 0, half], yrecv.at[layer, 0, half],
                y_send.at[layer, 0, half], y_recv.at[layer, 0, half], ymates[half],
            )
            for half in range(2)
        ]
        for half in range(2):
            hops[half].wait_recv()
            ysend[layer, 1, half] = ysend[layer, 0, half] + yrecv[layer, 0, half]
            hops[half] = remote(
                ysend.at[layer, 1, half], yrecv.at[layer, 1, half],
                y_send.at[layer, 1, half], y_recv.at[layer, 1, half], ymates[1 - half],
            )
        for half in range(2):
            hops[half].wait_recv()
            rows = slice(half * 8, half * 8 + 8)
            branch = (ysend[layer, 1, half].astype(F32) + yrecv[layer, 1, half].astype(F32)) * dscale[layer : layer + 1, :]
            old = stream[rows].reshape(TOK // 2, W).astype(F32)
            stream[rows] = (residual_keep * old + branch).astype(BF16).reshape(8, ROWS, W)
    here = pl.ds(c * 16, 16)
    mine = pltpu.make_async_copy(stream, out.at[here], out_sem.at[0])
    mine.start()
    last = remote(stream, out.at[here], out_sem.at[1], out_sem.at[2], peer)
    mine.wait()
    last.wait_recv()
    for copy in sent:
        copy.wait_send()


def gather(layer, step, k, hid, bits, mates, cb, ag_send, ag_recv, remote):
    fixed = ORDER[k][: step + 1]
    index = (layer, *(bits[i] if i in fixed else slice(None) for i in range(4)))
    return remote(
        hid[k].at[index], hid[k].at[index],
        ag_send.at[layer, step, k], ag_recv.at[layer, step, k], (mates[ORDER[k][step]], cb),
    )


def shards(tokens, *rest):
    vm = pltpu.VMEM
    dma = pltpu.SemaphoreType.DMA
    scratch = [
        vm((16, ROWS, W), BF16),
        vm((2, 2, 2, 2, ROWS, 128), F32),
        vm((2, 2, 2, 2, ROWS, W), BF16),
        vm((LAYERS, W), F32),
        vm((LAYERS, W), F32),
        vm((LAYERS, 2, W, FFD), F32),
        vm((LAYERS, FFD, W), F32),
        *(vm((LAYERS, 2, W, PRE[i]), BF16) for i in range(2)),
        *(vm((LAYERS, 2, HID[i], W), BF16) for i in range(2)),
        *(vm((2, LAYERS, FFD), F32) for _ in range(2)),
        *(vm((2, LAYERS, TAPS, FFD), F32) for _ in range(2)),
        *(vm((2, LAYERS, FFD), F32) for _ in range(2)),
    ]
    for _ in range(3):
        for step in range(4):
            for k in CH:
                scratch.append(vm((LAYERS, *(2,) * (3 - step), ROWS, PRE[k]), BF16))
    scratch += [vm((LAYERS, 2, 2, 2, 2, ROWS, HID[k]), BF16) for k in CH]
    scratch += [vm((TOK, W), F32), vm((LAYERS, 2, 2, TOK // 2, W), BF16), vm((LAYERS, 2, 2, TOK // 2, W), BF16)]
    scratch += [
        dma((16,)), dma((16,)), dma((16,)),
        dma((LAYERS, 4, 4)), dma((LAYERS, 4, 4)), dma((LAYERS, 4, 4)), dma((LAYERS, 4, 4)),
        dma((LAYERS, 2, 2)), dma((LAYERS, 2, 2)), dma((3,)),
    ]
    count = tokens.shape[0]
    result = pl.pallas_call(
        kernel,
        out_shape=jax.ShapeDtypeStruct((count // ROWS, ROWS, W), BF16),
        in_specs=[pl.BlockSpec(memory_space=pl.ANY)] * 12,
        out_specs=pl.BlockSpec(memory_space=pl.ANY),
        scratch_shapes=scratch,
        compiler_params=pltpu.CompilerParams(
            collective_id=0, has_side_effects=True, vmem_limit_bytes=60 * 1024 * 1024
        ),
        name="two_layers",
    )(tokens.reshape(count // ROWS, ROWS, W), *rest)
    return result.reshape(count, W)


def solution(mesh):
    placed = (
        P(None, "ra"),
        P(None, "ra"),
        P(None, "ra", "cb"),
        P(None, "cb"),
        P(None, "ra", "cb"),
        P(None, "cb"),
        P(None, None, "cb"),
        P(None, None, "cb"),
        P(None, "cb"),
        P(None, "cb"),
        P(None, "cb", "ra"),
        P(None, "ra"),
    )
    return jax.shard_map(
        shards, mesh=mesh, in_specs=placed, out_specs=P(None, "ra"), check_vma=False
    )
```

```python
import jax
import jax.numpy as jnp
from jax import lax
from jax.experimental import pallas as pl
from jax.experimental.pallas import tpu as pltpu
from jax.sharding import PartitionSpec as P

D = 3072
TAPS = 3
LAYERS = 2
SEQ_LEN = 8
epsilon = 1e-06
residual_keep = 0.5

MESH = pl.DeviceIdType.MESH
F32 = jnp.float32
BF16 = jnp.bfloat16

STREAMS = 2
TOK = 128
ROWS = 8
W = 192
FFD = 1056
MAIN = 512
LEFT = FFD - 2 * MAIN
PRE = (2 * MAIN + 128, 2 * MAIN, 2 * MAIN + 128, 2 * MAIN)
HID = (MAIN + 128, MAIN, MAIN + 128, MAIN)
ORDER = ((0, 1, 2, 3), (1, 0, 3, 2), (2, 3, 0, 1), (3, 2, 1, 0))
CH = range(4)
ST = range(STREAMS)


def pick(axis, index, rank):
    return tuple(index if i == axis else slice(None) for i in range(rank))


def kernel(
    tokens,
    norm_gain,
    gate_weight,
    gate_scale,
    value_weight,
    value_scale,
    gate_conv,
    value_conv,
    gate_bias,
    value_bias,
    down_weight,
    down_scale,
    out,
    *scratch,
):
    it = iter(scratch)
    take = lambda n: [next(it) for _ in range(n)]
    (stream, squares, normed, gain, dscale) = take(5)
    (wide, dwide) = take(2)
    wcols = take(2)
    drows = take(2)
    params = take(6)
    snd = [take(4) for _ in range(2)]
    kept = [take(4) for _ in range(2)]
    got = [take(4) for _ in range(2)]
    quad = take(4)
    pieces = take(4)
    hid = take(4)
    (total, ypart) = take(2)
    (load_sem, peer_send, peer_recv, rs_send, rs_recv, dx_send, dx_recv, ag_send, ag_recv, y_send, y_recv, out_sem) = take(12)

    ra = lax.axis_index("ra")
    cb = lax.axis_index("cb")
    x, z = ra % 4, ra // 4
    y, c = cb // 2, cb % 2

    def at(nx, nz):
        return nz * 4 + nx

    def flip(v):
        return v + 1 - 2 * (v % 2)

    def choose(first, second):
        return first * (1 - c) + second * c

    xa, xb, za, zb = at(flip(x), z), at(3 - x, z), at(x, flip(z)), at(x, 3 - z)
    xo, zo = at((x + 2) % 4, z), at(x, (z + 2) % 4)
    bxa, bxb, bza, bzb = ((x + 1) // 2) % 2, x // 2, ((z + 1) // 2) % 2, z // 2
    mates = (choose(xa, zb), choose(xb, za), choose(za, xb), choose(zb, xa))
    bits = (choose(bxa, bzb), choose(bxb, bza), choose(bza, bxb), choose(bzb, bxa))
    across = (choose(xo, zo), choose(zo, xo))
    peer = (ra, y * 2 + 1 - c)
    ymates = ((ra, flip(y) * 2 + c), (ra, (3 - y) * 2 + c), (ra, ((y + 2) % 4) * 2 + c))

    def ring(first, second):
        return (mates[first], cb), (mates[second], cb), (across[first // 2], cb)

    sources = (gate_scale, value_scale, gate_conv, value_conv, gate_bias, value_bias)
    loads = {}

    def load(name, src, dst, index):
        loads[name] = pltpu.make_async_copy(src, dst, load_sem.at[index])
        loads[name].start()

    for s in ST:
        load(("x", s), tokens.at[:, pl.ds(pl.multiple_of(c * 256 + s * TOK, TOK), TOK)], stream.at[s], s)
    load("gain", norm_gain, gain, 2)
    for layer in range(LAYERS):
        load(("g", layer), gate_weight.at[layer], wide.at[layer, 0], 3 + layer * 3)
        load(("v", layer), value_weight.at[layer], wide.at[layer, 1], 4 + layer * 3)
        load(("d", layer), down_weight.at[layer], dwide.at[layer], 5 + layer * 3)
        if layer == 0:
            load("ds", down_scale, dscale, 9)
            for i, src in enumerate(sources):
                load(("p", i), src, params[i].at[0], 10 + i)

    barrier = pltpu.get_barrier_semaphore()
    greet = [(m, cb) for m in (*mates, *across)] + [peer, *ymates]
    for target in greet:
        pl.semaphore_signal(barrier, inc=1, device_id=target, device_id_type=MESH)

    sent = []

    def remote(src, dst, send_sem, recv_sem, target):
        copy = pltpu.make_async_remote_copy(
            src_ref=src, dst_ref=dst, send_sem=send_sem, recv_sem=recv_sem,
            device_id=target, device_id_type=MESH,
        )
        copy.start()
        sent.append(copy)
        return copy

    line = lax.broadcasted_iota(jnp.int32, (LEFT, 128), 1)
    row = lax.broadcasted_iota(jnp.int32, (LEFT, 128), 0)
    put_gate = (line == row).astype(F32).astype(BF16)
    put_value = (line == row + LEFT).astype(F32).astype(BF16)

    def cast_up(layer):
        loads[("g", layer)].wait()
        loads[("v", layer)].wait()
        g, v = wide.at[layer, 0], wide.at[layer, 1]
        wcols[0][layer, 0, :, 0:MAIN] = g[:, 0:MAIN].astype(BF16)
        wcols[0][layer, 0, :, MAIN : 2 * MAIN] = v[:, 0:MAIN].astype(BF16)
        low = jnp.dot(g[:, 2 * MAIN : FFD].astype(BF16), put_gate, preferred_element_type=F32)
        low += jnp.dot(v[:, 2 * MAIN : FFD].astype(BF16), put_value, preferred_element_type=F32)
        wcols[0][layer, 0, :, 2 * MAIN : 2 * MAIN + 128] = low.astype(BF16)
        wcols[1][layer, 0, :, 0:MAIN] = g[:, MAIN : 2 * MAIN].astype(BF16)
        wcols[1][layer, 0, :, MAIN : 2 * MAIN] = v[:, MAIN : 2 * MAIN].astype(BF16)

    def cast_down(layer):
        loads[("d", layer)].wait()
        d = dwide.at[layer]
        drows[0][layer, 0, :, 0:MAIN] = d[:, 0:MAIN].astype(BF16)
        low = jnp.dot(d[:, 2 * MAIN : FFD].astype(BF16), put_gate, preferred_element_type=F32)
        drows[0][layer, 0, :, MAIN : MAIN + 128] = low.astype(BF16)
        drows[1][layer, 0, :, :] = d[:, MAIN : 2 * MAIN].astype(BF16)

    from_peer = {}

    def give(name, ref_from, ref_to, index):
        from_peer[name] = remote(ref_from, ref_to, peer_send.at[index], peer_recv.at[index], peer)

    def need(name):
        if name in from_peer:
            from_peer.pop(name).wait_recv()

    lane = lax.broadcasted_iota(jnp.int32, (TOK, 128), 1)

    def prepare(layer, s):
        values = jnp.transpose(stream[s].astype(F32))
        own = jnp.sum(values * values, axis=1, keepdims=True)
        squares[s] = jnp.where(lane == 2 * LEFT, own, 0.0).reshape(squares.shape[1:])
        rounded = (values * gain[layer : layer + 1, :]).astype(BF16).astype(F32)
        normed[s] = rounded.reshape(normed.shape[1:])

    def project(ref, layer, s, k, index):
        rows = normed[(s, *index)].reshape(TOK // 2, W).astype(BF16)
        product = jnp.dot(rows, wcols[k % 2][layer, k // 2], preferred_element_type=F32)
        if k == 0:
            tail = product[:, 2 * MAIN :] + squares[(s, *index)].reshape(TOK // 2, 128)
            ref[..., 2 * MAIN :] = tail.reshape(2, 2, 2, ROWS, 128).astype(BF16)
            ref[..., 0 : 2 * MAIN] = product[:, : 2 * MAIN].reshape(2, 2, 2, ROWS, 2 * MAIN).astype(BF16)
        else:
            ref[...] = product.reshape(2, 2, 2, ROWS, PRE[k]).astype(BF16)

    def halve(layer, s, step, k):
        return remote(
            snd[step][k].at[layer, s], got[step][k].at[layer, s],
            rs_send.at[layer, s, step, k], rs_recv.at[layer, s, step, k], (mates[ORDER[k][step]], cb),
        )

    keep_row = lax.broadcasted_iota(jnp.int32, (ROWS, 1), 0)

    def mix(pre, taps, bias):
        back_one = jnp.where(keep_row >= 1, pltpu.roll(pre, 1, 0), 0.0)
        back_two = jnp.where(keep_row >= 2, pltpu.roll(pre, 2, 0), 0.0)
        return bias + back_two * taps[0] + back_one * taps[1] + pre * taps[2]

    def gated(layer, slot, cols, gate_sum, value_sum, inverse):
        scale_g, scale_v, conv_g, conv_v, bias_g, bias_v = params
        one = lambda ref: ref[slot, layer : layer + 1, cols]
        taps = lambda ref: [ref[slot, i, layer : layer + 1, cols] for i in range(TAPS)]
        gate = mix(gate_sum * inverse * one(scale_g), taps(conv_g), one(bias_g))
        value = mix(value_sum * inverse * one(scale_v), taps(conv_v), one(bias_v))
        return (gate / (1.0 + jnp.exp(-gate)) * value).astype(BF16)

    flights = {}

    def first(layer, s, k):
        if k >= 2:
            need(("w", k - 2, layer))
        dim = ORDER[k][0]
        project(snd[0][k].at[layer, s], layer, s, k, pick(dim, 1 - bits[dim], 4))
        flights[s, k] = halve(layer, s, 0, k)

    def own_half(layer, s, k):
        dim = ORDER[k][0]
        project(kept[0][k].at[layer, s], layer, s, k, pick(dim, bits[dim], 4))

    def second(layer, s, k):
        left = sorted(ORDER[k][1:])
        dim = ORDER[k][1]
        axis = left.index(dim)
        flights[s, k].wait_recv()
        away, home = pick(axis, 1 - bits[dim], 3), pick(axis, bits[dim], 3)
        before, arrived = kept[0][k].at[layer, s], got[0][k].at[layer, s]
        snd[1][k][layer, s] = before[away] + arrived[away]
        flights[s, k] = halve(layer, s, 1, k)
        kept[1][k][layer, s] = before[home] + arrived[home]

    def third(layer, s, k):
        low, high = sorted(ORDER[k][2:])
        flights[s, k].wait_recv()
        quad[k][layer, s] = kept[1][k][layer, s] + got[1][k][layer, s]
        blocks = ((1 - bits[low], bits[high]), (bits[low], 1 - bits[high]), (1 - bits[low], 1 - bits[high]))
        flights[s, k] = [
            remote(
                quad[k].at[(layer, s, *blocks[i])], pieces[k].at[layer, s, i],
                dx_send.at[layer, s, k, i], dx_recv.at[layer, s, k, i], target,
            )
            for i, target in enumerate(ring(low, high))
        ]

    inverse = {}

    def spread(layer, s, k, number, index, targets):
        place = (layer, s, *index)
        return [
            remote(
                hid[k].at[place], hid[k].at[place],
                ag_send.at[layer, s, k, number + i], ag_recv.at[layer, s, k, number + i], target,
            )
            for i, target in enumerate(targets)
        ]

    def activate(layer, s, k):
        slot, part = k // 2, k % 2
        low_dim, high_dim = sorted(ORDER[k][2:])
        for copy in flights[s, k]:
            copy.wait_recv()
        final = quad[k][layer, s, bits[low_dim], bits[high_dim]].astype(F32)
        for i in range(3):
            final = final + pieces[k][layer, s, i].astype(F32)
        if k == 0:
            tail = final[:, 2 * MAIN :]
            own_lane = lax.broadcasted_iota(jnp.int32, (ROWS, 128), 1) == 2 * LEFT
            mean = jnp.sum(jnp.where(own_lane, tail, 0.0), axis=1, keepdims=True) / D
            inverse[s] = lax.rsqrt(mean + epsilon)
        place = (layer, s, *bits, slice(None))
        cols = slice(part * MAIN, (part + 1) * MAIN)
        hid[k][(*place, slice(0, MAIN))] = gated(
            layer, slot, cols, final[:, 0:MAIN], final[:, MAIN : 2 * MAIN], inverse[s]
        )
        if part == 0:
            tail = final[:, 2 * MAIN :]
            turned = pltpu.roll(tail, 128 - LEFT, 1)
            hid[k][(*place, slice(MAIN, MAIN + 128))] = jnp.zeros((ROWS, 128), BF16)
            hid[k][(*place, slice(MAIN, MAIN + LEFT))] = gated(
                layer, slot, slice(2 * MAIN, FFD), tail[:, 0:LEFT], turned[:, 0:LEFT], inverse[s]
            )
        near = ring(low_dim, high_dim)
        far = ring(*sorted(ORDER[k][:2]))
        flights[s, k] = spread(layer, s, k, 0, bits, near), spread(layer, s, k, 3, bits, far)

    def forward(layer, s, k):
        low, high = sorted(ORDER[k][2:])
        near, far = flights[s, k]
        targets = ring(*sorted(ORDER[k][:2]))
        near[1].wait_recv()
        index = tuple(1 - bits[i] if i == high else bits[i] for i in range(4))
        one = spread(layer, s, k, 6, index, targets)
        near[0].wait_recv()
        near[2].wait_recv()
        index = tuple(1 - bits[i] if i == low else slice(None) if i == high else bits[i] for i in range(4))
        two = spread(layer, s, k, 9, index, targets)
        flights[s, k] = [*far, *one, *two]

    def lower(layer, s):
        for k in CH:
            if k >= 2:
                need(("d", k - 2, layer))
            for copy in flights[s, k]:
                copy.wait_recv()
            part = lax.dot_general(
                drows[k % 2][layer, k // 2],
                hid[k].at[layer, s].reshape(TOK, HID[k])[...],
                (((1,), (1,)), ((), ())),
                preferred_element_type=F32,
            )
            if k == 0:
                total[...] = part
            elif k < 3:
                total[...] += part
            else:
                ypart[layer, s, y] = (total[...] + part).astype(BF16)
        flights[s] = [
            remote(
                ypart.at[layer, s, y], ypart.at[layer, s, y],
                y_send.at[layer, s, i], y_recv.at[layer, s, i], target,
            )
            for i, target in enumerate(ymates)
        ]

    def close(layer, s, scale):
        for copy in flights[s]:
            copy.wait_recv()
        branch = ypart[layer, s, 0].astype(F32)
        for i in range(1, 4):
            branch = branch + ypart[layer, s, i].astype(F32)
        stream[s] = (residual_keep * stream[s].astype(F32) + branch * scale).astype(BF16)

    loads["gain"].wait()
    for layer in range(LAYERS):
        if layer == 0:
            for s in ST:
                loads[("x", s)].wait()
                prepare(0, s)
            cast_up(0)
            pl.semaphore_wait(barrier, len(greet))
            for i in range(2):
                give(("w", i, 0), wcols[i].at[0, 0], wcols[i].at[0, 1], i)
            turns = [(s, k) for half in ((0, 1), (2, 3)) for s in ST for k in half]
            for s, k in turns:
                first(0, s, k)
            for s, k in turns:
                own_half(0, s, k)
            for i in range(6):
                loads[("p", i)].wait()
                give(("p", i), params[i].at[0], params[i].at[1], 8 + i)
            cast_down(0)
            for i in range(2):
                give(("d", i, 0), drows[i].at[0, 0], drows[i].at[0, 1], 4 + i)
            loads["ds"].wait()
        else:
            turns = [(s, k) for s in ST for k in CH]
            for s in ST:
                close(0, s, scale)
                prepare(1, s)
                for k in CH:
                    first(1, s, k)
            for s, k in turns:
                own_half(1, s, k)
        scale = jnp.transpose(jnp.broadcast_to(dscale[layer : layer + 1, :], (TOK, W)))
        for s, k in turns:
            second(layer, s, k)
        if layer == 0:
            cast_up(1)
            for i in range(2):
                give(("w", i, 1), wcols[i].at[1, 0], wcols[i].at[1, 1], 2 + i)
        for s, k in turns:
            third(layer, s, k)
        if layer == 0:
            cast_down(1)
            for i in range(2):
                give(("d", i, 1), drows[i].at[1, 0], drows[i].at[1, 1], 6 + i)
            for i in range(6):
                need(("p", i))
        for s, k in turns:
            activate(layer, s, k)
        for s, k in turns:
            forward(layer, s, k)
        for s in ST:
            lower(layer, s)
    ends = []
    for s in ST:
        close(1, s, scale)
        here = pl.ds(pl.multiple_of(c * 256 + s * TOK, TOK), TOK)
        mine = pltpu.make_async_copy(stream.at[s], out.at[:, here], out_sem.at[s])
        mine.start()
        ends.append((mine, remote(stream.at[s], out.at[:, here], out_sem.at[2 + s], out_sem.at[4 + s], peer)))
    for mine, theirs in ends:
        mine.wait()
        theirs.wait_recv()
    for copy in sent:
        copy.wait_send()


def shards(tokens, norm_gain, gate_weight, gate_scale, value_weight, value_scale, gate_conv, value_conv, *rest):
    gate_bias, value_bias, down_weight, down_scale = rest
    vm = pltpu.VMEM
    dma = pltpu.SemaphoreType.DMA
    lead = (LAYERS, STREAMS)
    scratch = [
        vm((STREAMS, W, TOK), BF16),
        vm((STREAMS, 2, 2, 2, 2, ROWS, 128), F32),
        vm((STREAMS, 2, 2, 2, 2, ROWS, W), F32),
        vm((LAYERS, W), F32),
        vm((LAYERS, W), F32),
        vm((LAYERS, 2, W, FFD), F32),
        vm((LAYERS, W, FFD), F32),
        *(vm((LAYERS, 2, W, PRE[i]), BF16) for i in range(2)),
        *(vm((LAYERS, 2, W, HID[i]), BF16) for i in range(2)),
        *(vm((2, LAYERS, FFD), F32) for _ in range(2)),
        *(vm((2, TAPS, LAYERS, FFD), F32) for _ in range(2)),
        *(vm((2, LAYERS, FFD), F32) for _ in range(2)),
    ]
    for _ in range(3):
        for step in range(2):
            for k in CH:
                scratch.append(vm((*lead, *(2,) * (3 - step), ROWS, PRE[k]), BF16))
    scratch += [vm((*lead, 2, 2, ROWS, PRE[k]), BF16) for k in CH]
    scratch += [vm((*lead, 3, ROWS, PRE[k]), BF16) for k in CH]
    scratch += [vm((*lead, 2, 2, 2, 2, ROWS, HID[k]), BF16) for k in CH]
    scratch += [vm((W, TOK), F32), vm((*lead, 4, W, TOK), BF16)]
    scratch += [
        dma((16,)), dma((16,)), dma((16,)),
        dma((*lead, 2, 4)), dma((*lead, 2, 4)),
        dma((*lead, 4, 3)), dma((*lead, 4, 3)),
        dma((*lead, 4, 12)), dma((*lead, 4, 12)),
        dma((*lead, 3)), dma((*lead, 3)), dma((6,)),
    ]
    result = pl.pallas_call(
        kernel,
        out_shape=jax.ShapeDtypeStruct((W, tokens.shape[0]), BF16),
        in_specs=[pl.BlockSpec(memory_space=pl.ANY)] * 12,
        out_specs=pl.BlockSpec(memory_space=pl.ANY),
        scratch_shapes=scratch,
        compiler_params=pltpu.CompilerParams(
            collective_id=0, has_side_effects=True, vmem_limit_bytes=60 * 1024 * 1024
        ),
        name="two_layers",
    )(
        tokens.T, norm_gain, gate_weight, gate_scale, value_weight, value_scale,
        gate_conv.transpose(1, 0, 2), value_conv.transpose(1, 0, 2), gate_bias, value_bias,
        down_weight.transpose(0, 2, 1), down_scale,
    )
    return result.T


def solution(mesh):
    placed = (
        P(None, "ra"),
        P(None, "ra"),
        P(None, "ra", "cb"),
        P(None, "cb"),
        P(None, "ra", "cb"),
        P(None, "cb"),
        P(None, None, "cb"),
        P(None, None, "cb"),
        P(None, "cb"),
        P(None, "cb"),
        P(None, "cb", "ra"),
        P(None, "ra"),
    )
    return jax.shard_map(
        shards, mesh=mesh, in_specs=placed, out_specs=P(None, "ra"), check_vma=False
    )
```
